32 devices in a mesh: sp: 8 (over z, x), tp: 4 (over y, core).
Axes of the slice: x: 2, y: 2, z: 4, core: 2. Of those that a mesh axis runs over, the one named last changes fastest.
Arguments:
- resid: bfloat16 [2048, 4096], P('sp'), may hold values from -6 to 6
- queries: bfloat16 [2048, 3072], P('sp', 'tp'), may hold values from -1000 to 1000
- latent: bfloat16 [2048, 512], P('sp'), may hold values from -6 to 6
- rope_key: bfloat16 [2048, 64], P('sp'), may hold values from -6 to 6
- lat_gain: float32 [512], replicated, may hold values from 0.1 to 1.9
- kv_weight: bfloat16 [512, 4096], P(None, 'tp'), may hold values from -4 to 4
- out_gain: float32 [2048], P('tp'), may hold values from 0.1 to 1.9
- out_weight: bfloat16 [2048, 4096], P('tp'), may hold values from -0.125 to 0.125
- ffn_gain: float32 [4096], replicated, may hold values from 0.1 to 1.9
- gate_weight: bfloat16 [4096, 6144], P('sp', 'tp'), may hold values from -0.09375 to 0.09375
- up_weight: bfloat16 [4096, 6144], P('sp', 'tp'), may hold values from -0.09375 to 0.09375
- down_weight: bfloat16 [6144, 4096], P('tp', 'sp'), may hold values from -0.078125 to 0.078125
Outputs:
- result: bfloat16 [2048, 4096], P(('sp', 'tp'))
The draws below stay inside these ranges and needn't reach their ends.
All inputs are finite; a program needn't handle non-finite values.
Results may differ from the reference program's by a relative error of at most 0.018.
Values may be sent and summed in bfloat16 or wider, within the bound.
A program may use at most 192 MiB of HBM per device.

```python
import math
import jax
import jax.numpy as jnp
from jax import lax

D = 4096
HEADS = 16
NOPE = 128
ROPE = 64
VDIM = 128
KV_RANK = 512
FF = 6144
TOK_DEV = 256
TOKENS = 2048
N_TP = 4


def draw_pair(key):
    base = jax.random.fold_in(key, 7)
    key_one, key_two = jax.random.split(base, 2)
    width = NOPE + ROPE
    query = jax.random.truncated_normal(key_one, -6.0, 6.0, (TOKENS, HEADS, width), jnp.float32)
    rotary = jax.random.truncated_normal(key_two, -4.0, 4.0, (TOKENS, ROPE), jnp.float32)
    return (query.reshape(TOKENS, HEADS * width), rotary)


def draw_queries(key, part):
    return draw_pair(key)[0].astype(jnp.bfloat16)


def draw_rope_key(key, part):
    return draw_pair(key)[1].astype(jnp.bfloat16)


def draw_kv_weight(key, part):
    base = jax.random.fold_in(key, 11)
    shape = (KV_RANK, HEADS, NOPE + VDIM)
    matrix = jax.random.truncated_normal(base, -6.0, 6.0, shape, jnp.float32)
    ceiling = 3.0
    factor = ceiling ** (jnp.arange(HEADS, dtype=jnp.float32) / (HEADS - 1))
    scaled = jnp.concatenate([matrix[:, :, :NOPE], matrix[:, :, NOPE:] * factor[None, :, None]], axis=-1)
    return (scaled / math.sqrt(KV_RANK)).reshape(KV_RANK, HEADS * (NOPE + VDIM)).astype(jnp.bfloat16)


def shard_levels(rng, shape, pieces, low, top_value):
    level, own = 1.0, jax.random.fold_in(rng, 6)
    for dim, shards_of in pieces:
        heights = jnp.exp(jax.random.uniform(jax.random.fold_in(own, dim), (shards_of,), jnp.float32, low / len(pieces), top_value / len(pieces)))
        level = level * jnp.repeat(heights, shape[dim] // shards_of).reshape([-1 if axis == dim else 1 for axis in range(len(shape))])
    return level


def noise(own_key, dims, scale, reach, shards=(), kind=jnp.bfloat16):
    values = scale * jax.random.normal(own_key, dims, jnp.float32)
    if shards:
        values = values * shard_levels(own_key, dims, shards, -0.22, 0.18)
    return jnp.clip(values, -reach, reach).astype(kind)


def setup_inputs(seed: int = 0) -> dict:
    streams_of = jax.random.split(jax.random.key(seed), 13)
    return {
        "resid": noise(streams_of[0], (TOKENS, D), 1.0, 6.0, ((0, 8),)),
        "queries": draw_queries(jax.random.fold_in(streams_of[12], 71), 0),
        "latent": noise(streams_of[2], (TOKENS, KV_RANK), 1.0, 6.0, ((0, 8),)),
        "rope_key": draw_rope_key(jax.random.fold_in(streams_of[12], 71), 0),
        "lat_gain": jnp.clip(1.0 + 0.18 * jax.random.normal(streams_of[4], (KV_RANK,), jnp.float32), 0.1, 1.9),
        "kv_weight": draw_kv_weight(jax.random.fold_in(streams_of[12], 71), 0),
        "out_gain": jnp.clip(1.0 + 0.18 * jax.random.normal(streams_of[6], (HEADS * VDIM,), jnp.float32), 0.1, 1.9),
        "out_weight": noise(streams_of[7], (HEADS * VDIM, D), (HEADS * VDIM) ** -0.5, 0.125, ((0, 4),)),
        "ffn_gain": jnp.clip(1.0 + 0.18 * jax.random.normal(streams_of[8], (D,), jnp.float32), 0.1, 1.9),
        "gate_weight": noise(streams_of[9], (D, FF), D ** -0.5, 0.09375, ((0, 8), (1, 4))),
        "up_weight": noise(streams_of[10], (D, FF), D ** -0.5, 0.09375, ((0, 8), (1, 4))),
        "down_weight": noise(streams_of[11], (FF, D), FF ** -0.5, 0.078125, ((0, 4), (1, 8))),
    }


EPSILON = 1e-06
THETA = 10000.0

def rotate(values, places):
    half = values.shape[-1] // 2
    inverse = THETA ** (-jnp.arange(half, dtype=jnp.float32) / half)
    angle = places[..., None] * inverse
    cosine = jnp.cos(angle)
    sine = jnp.sin(angle)
    first = values[..., :half]
    second = values[..., half:]
    return jnp.concatenate([first * cosine - second * sine, first * sine + second * cosine], axis=-1)

def norm_rows(values, gain):
    wide = values.astype(jnp.float32)
    return wide * lax.rsqrt(lax.optimization_barrier(jnp.mean(wide * wide, axis=-1, keepdims=True)) + EPSILON) * gain.astype(jnp.float32)

def round_trip(values):
    return lax.optimization_barrier(values.astype(jnp.bfloat16)).astype(jnp.float32)

def reference(resid, queries, latent, rope_key, lat_gain, kv_weight, out_gain, out_weight, ffn_gain, gate_weight, up_weight, down_weight):
    total_rows = latent.shape[0]
    positions = jnp.arange(total_rows, dtype=jnp.int32)
    places = positions.astype(jnp.float32)
    normed = norm_rows(latent, lat_gain).astype(jnp.bfloat16)
    key_value = jnp.dot(normed, kv_weight, preferred_element_type=jnp.float32).astype(jnp.bfloat16)
    key_value = key_value.reshape(total_rows, HEADS, NOPE + VDIM).astype(jnp.float32)
    key_nope = key_value[:, :, :NOPE]
    values = key_value[:, :, NOPE:]
    key_rope = round_trip(rotate(rope_key.astype(jnp.float32), places))
    query = queries.reshape(total_rows, HEADS, NOPE + ROPE)
    query_nope = query[:, :, :NOPE].astype(jnp.float32)
    query_rope = round_trip(rotate(query[:, :, NOPE:].astype(jnp.float32), places[:, None]))
    scale = 1.0 / math.sqrt(NOPE + ROPE)
    blocks = total_rows // TOK_DEV

    def attend_block(index):
        first = (index * TOK_DEV).astype(jnp.int32)
        block_nope = lax.dynamic_slice_in_dim(query_nope, first, TOK_DEV, 0)
        block_rope = lax.dynamic_slice_in_dim(query_rope, first, TOK_DEV, 0)
        scores = jnp.einsum('qhd,khd->hqk', block_nope, key_nope) + jnp.einsum('qhr,kr->hqk', block_rope, key_rope)
        scores = scores * scale
        query_index = first + jnp.arange(TOK_DEV, dtype=jnp.int32)
        allowed = (positions[None, :] <= query_index[:, None])[None]
        scores = jnp.where(allowed, scores, -jnp.inf)
        highest = lax.optimization_barrier(jnp.max(scores, axis=-1, keepdims=True))
        weights = jnp.where(allowed, jnp.exp(scores - highest), 0.0)
        totals = lax.optimization_barrier(jnp.sum(weights, axis=-1))
        mixed = jnp.einsum('hqk,khd->qhd', round_trip(weights), values)
        return (mixed / jnp.transpose(totals)[:, :, None]).astype(jnp.bfloat16)
    attended = lax.map(attend_block, jnp.arange(blocks, dtype=jnp.int32))
    attended = attended.reshape(total_rows, HEADS * VDIM)
    normed_out = norm_rows(attended, out_gain).astype(jnp.bfloat16)
    group_width = HEADS * VDIM // N_TP
    attn_sum = jnp.zeros((total_rows, D), jnp.float32)
    for group in range(N_TP):
        lower = group * group_width
        part = jnp.dot(normed_out[:, lower:lower + group_width], out_weight[lower:lower + group_width], preferred_element_type=jnp.float32)
        attn_sum = attn_sum + round_trip(part)
    middle = (resid.astype(jnp.float32) + attn_sum).astype(jnp.bfloat16)
    normed_mid = norm_rows(middle, ffn_gain).astype(jnp.bfloat16)
    gate = jnp.dot(normed_mid, gate_weight, preferred_element_type=jnp.float32)
    upward = jnp.dot(normed_mid, up_weight, preferred_element_type=jnp.float32)
    hidden = (jax.nn.silu(gate) * upward).astype(jnp.bfloat16)
    group_units = FF // N_TP
    ffn_sum = jnp.zeros((total_rows, D), jnp.float32)
    for group in range(N_TP):
        lower = group * group_units
        part = jnp.dot(hidden[:, lower:lower + group_units], down_weight[lower:lower + group_units], preferred_element_type=jnp.float32)
        ffn_sum = ffn_sum + round_trip(part)
    return (middle.astype(jnp.float32) + ffn_sum).astype(jnp.bfloat16)
```

```python
import math

import jax
import jax.numpy as jnp
from jax import lax
from jax.sharding import PartitionSpec as P


HEADS = 16
NOPE = 128
ROPE = 64
VDIM = 128


EPSILON = 1e-06
THETA = 10000.0
LOWEST = -1e30
GROUP = 4


def rotate(values, places):
    half = values.shape[-1] // 2
    inverse = THETA ** (-jnp.arange(half, dtype=jnp.float32) / half)
    angle = places[..., None] * inverse
    cosine = jnp.cos(angle)
    sine = jnp.sin(angle)
    first = values[..., :half]
    second = values[..., half:]
    return jnp.concatenate(
        [first * cosine - second * sine, first * sine + second * cosine], axis=-1
    )


def norm_rows(values, gain):
    wide = values.astype(jnp.float32)
    return wide * lax.rsqrt(jnp.mean(wide * wide, axis=-1, keepdims=True) + EPSILON) * gain


def make_keys(latent_piece, rotary_piece, lat_gain, kv_weight):
    normed = norm_rows(latent_piece, lat_gain).astype(jnp.bfloat16)
    key_value = jnp.dot(normed, kv_weight, preferred_element_type=jnp.float32)
    key_value = key_value.astype(jnp.bfloat16)
    key_index = jnp.arange(latent_piece.shape[0], dtype=jnp.int32)
    key_rope = rotate(rotary_piece.astype(jnp.float32), key_index.astype(jnp.float32)).astype(
        jnp.bfloat16
    )
    return (key_value, key_rope)


def to_near(values, flip):
    ranks = lax.axis_size("sp")
    return lax.ppermute(values, "sp", [(rank, rank ^ flip) for rank in range(ranks)])


def to_high(values, step, ranks):
    if step % (ranks // GROUP) == 0:
        return values
    return lax.ppermute(
        values, "sp", [(rank, (rank + step * GROUP) % ranks) for rank in range(ranks)]
    )


def by_distance(values, place):
    blocks = jnp.split(values, GROUP, axis=1)
    blocks = [jnp.where(place % 2 == 1, blocks[j ^ 1], blocks[j]) for j in range(GROUP)]
    blocks = [jnp.where(place // 2 == 1, blocks[j ^ 2], blocks[j]) for j in range(GROUP)]
    return jnp.concatenate(blocks, axis=1)


def near_weights(gate, up, down):
    gate_one = to_near(gate, 1)
    up_two = to_near(up, 2)
    up_one = to_near(up, 1)
    gate_two = to_near(gate, 2)
    gate_both = to_near(gate_one, 2)
    up_both = to_near(up_two, 1)
    down, gate_both, up_both = lax.optimization_barrier((down, gate_both, up_both))
    half = down.shape[0] // 2
    down_one = to_near(down, 1)
    down_two = to_near(down, 2)
    down_both = jnp.concatenate([to_near(down_one[:half], 2), to_near(down_two[half:], 1)], axis=0)
    return (
        (gate, gate_one, gate_two, gate_both),
        (up, up_one, up_two, up_both),
        (down, down_one, down_two, down_both),
    )


def blocks_dot(rows, weights, block):
    return sum(
        jnp.dot(
            rows[:, place * block : (place + 1) * block], weight, preferred_element_type=jnp.float32
        )
        for place, weight in enumerate(weights)
    )


def body(
    resid,
    queries,
    latent,
    rope_key,
    lat_gain,
    kv_weight,
    out_gain,
    out_weight,
    ffn_gain,
    gate_weight,
    up_weight,
    down_weight,
):
    gate_blocks, up_blocks, down_blocks = near_weights(gate_weight, up_weight, down_weight)
    rows_here = resid.shape[0]
    first_row = lax.axis_index("sp") * rows_here
    heads_here = queries.shape[1] // (NOPE + ROPE)
    query = queries.reshape(rows_here, heads_here, NOPE + ROPE)
    query_index = first_row + jnp.arange(rows_here, dtype=jnp.int32)
    query_nope = query[:, :, :NOPE]
    query_rope = rotate(
        query[:, :, NOPE:].astype(jnp.float32), query_index.astype(jnp.float32)[:, None]
    ).astype(jnp.bfloat16)
    scale = 1.0 / math.sqrt(NOPE + ROPE)

    def accumulate(state, key_value, key_rope):
        running_max, running_sum, weighted = state
        length = key_value.shape[0]
        key_value = key_value.reshape(length, heads_here, NOPE + VDIM)
        key_index = jnp.arange(length, dtype=jnp.int32)
        scores = jnp.einsum(
            "qhd,khd->hqk", query_nope, key_value[:, :, :NOPE], preferred_element_type=jnp.float32
        )
        scores = (
            scores
            + jnp.einsum("qhr,kr->hqk", query_rope, key_rope, preferred_element_type=jnp.float32)
        ) * scale
        allowed = (key_index[None, :] <= query_index[:, None])[None]
        scores = jnp.where(allowed, scores, LOWEST)
        new_max = jnp.maximum(running_max, jnp.max(scores, axis=-1))
        weights = jnp.where(allowed, jnp.exp(scores - new_max[:, :, None]), 0.0)
        running_sum = jnp.sum(weights, axis=-1)
        added = jnp.einsum(
            "hqk,khd->qhd",
            weights.astype(jnp.bfloat16),
            key_value[:, :, NOPE:],
            preferred_element_type=jnp.float32,
        )
        weighted = added
        return (new_max, running_sum, weighted)

    initial = (
        jnp.full((heads_here, rows_here), LOWEST, jnp.float32),
        jnp.zeros((heads_here, rows_here), jnp.float32),
        jnp.zeros((rows_here, heads_here, VDIM), jnp.float32),
    )
    both = lax.all_gather(
        jnp.concatenate([latent, rope_key], axis=1), "sp", axis=0, tiled=True
    )
    pieces = (both[:, : latent.shape[1]], both[:, latent.shape[1] :])

    def update(state):
        key_value, key_rope = make_keys(pieces[0], pieces[1], lat_gain, kv_weight)
        return accumulate(state, key_value, key_rope)

    _, running_sum, weighted = update(initial)
    attended = (weighted / jnp.transpose(running_sum)[:, :, None]).astype(jnp.bfloat16)
    attended_float = attended.reshape(rows_here, heads_here * VDIM).astype(jnp.float32)
    squares = lax.psum(jnp.sum(attended_float * attended_float, axis=1), "tp")
    normed_out = attended_float * lax.rsqrt(squares / (HEADS * VDIM) + EPSILON)[:, None] * out_gain
    normed_out = normed_out.astype(jnp.bfloat16)
    share = rows_here // lax.axis_size("tp")
    own_first = lax.axis_index("tp") * share
    projected = jnp.dot(normed_out, out_weight, preferred_element_type=jnp.float32)
    projected = projected.astype(jnp.bfloat16)
    attn_sum = lax.psum_scatter(
        projected,
        "tp",
        scatter_dimension=0,
        tiled=True,
    ).astype(jnp.float32)
    own_resid = lax.dynamic_slice_in_dim(resid, own_first, share, 0)
    middle = (own_resid.astype(jnp.float32) + attn_sum).astype(jnp.bfloat16)
    ranks = lax.axis_size("sp")
    highs = ranks // GROUP
    rank = lax.axis_index("sp")
    high = rank // GROUP
    place = rank % GROUP
    width = resid.shape[1]
    block = width // ranks
    wide = GROUP * block
    mids = norm_rows(middle, ffn_gain).astype(jnp.bfloat16)
    mids = [
        to_high(
            by_distance(
                lax.dynamic_slice_in_dim(mids, (high + step) % highs * wide, wide, 1), place
            ),
            step,
            ranks,
        )
        for step in range(highs)
    ]
    mids = lax.all_gather(jnp.concatenate(mids, axis=1), "tp", axis=0, tiled=True)
    gates, ups = None, None
    for step in list(range(1, highs)) + [0]:
        piece = mids[:, step * wide : (step + 1) * wide]
        gate = blocks_dot(piece, gate_blocks, block)
        up = blocks_dot(piece, up_blocks, block)
        if step:
            gate = to_high(gate.astype(jnp.bfloat16), highs - step, ranks).astype(jnp.float32)
            up = to_high(up.astype(jnp.bfloat16), highs - step, ranks).astype(jnp.float32)
        gates = gate if gates is None else gates + gate
        ups = up if ups is None else ups + up
    hidden = (jax.nn.silu(gates) * ups).astype(jnp.bfloat16)
    terms = []
    for step in range(highs):
        theirs = to_high(hidden, step, ranks)
        terms += [
            jnp.dot(theirs, weight, preferred_element_type=jnp.float32).astype(jnp.bfloat16)
            for weight in down_blocks
        ]
    terms = lax.psum_scatter(
        jnp.concatenate(terms, axis=1), "tp", scatter_dimension=0, tiled=True
    )
    terms = jnp.concatenate(
        [
            by_distance(
                to_high(terms[:, step * wide : (step + 1) * wide], highs - step, ranks), place
            )
            for step in range(highs)
        ],
        axis=1,
    )
    ffn_sum = jnp.concatenate(
        [
            lax.dynamic_slice_in_dim(terms, (index - high + highs) % highs * wide, wide, 1)
            for index in range(highs)
        ],
        axis=1,
    ).astype(jnp.float32)
    return (middle.astype(jnp.float32) + ffn_sum).astype(jnp.bfloat16)


def solution(mesh):
    placed = (
        P("sp", None),
        P("sp", "tp"),
        P("sp", None),
        P("sp", None),
        P(),
        P(None, "tp"),
        P("tp"),
        P("tp", None),
        P(),
        P("sp", "tp"),
        P("sp", "tp"),
        P("tp", "sp"),
    )

    return jax.shard_map(
        body, mesh=mesh, in_specs=placed, out_specs=P(("sp", "tp"), None), check_vma=False
    )
```

```python
import math

import jax
import jax.numpy as jnp
from jax import lax
from jax.sharding import PartitionSpec as P


HEADS = 16
NOPE = 128
ROPE = 64
VDIM = 128


EPSILON = 1e-06
THETA = 10000.0
LOWEST = -1e30
GROUP = 4


def rotate(values, places):
    half = values.shape[-1] // 2
    inverse = THETA ** (-jnp.arange(half, dtype=jnp.float32) / half)
    angle = places[..., None] * inverse
    cosine = jnp.cos(angle)
    sine = jnp.sin(angle)
    first = values[..., :half]
    second = values[..., half:]
    return jnp.concatenate(
        [first * cosine - second * sine, first * sine + second * cosine], axis=-1
    )


def norm_rows(values, gain):
    wide = values.astype(jnp.float32)
    return wide * lax.rsqrt(jnp.mean(wide * wide, axis=-1, keepdims=True) + EPSILON) * gain


def make_keys(latent_piece, rotary_piece, lat_gain, kv_weight, key_index):
    normed = norm_rows(latent_piece, lat_gain).astype(jnp.bfloat16)
    key_value = jnp.dot(normed, kv_weight, preferred_element_type=jnp.float32)
    key_value = key_value.astype(jnp.bfloat16)
    key_rope = rotate(rotary_piece.astype(jnp.float32), key_index.astype(jnp.float32)).astype(
        jnp.bfloat16
    )
    return (key_value, key_rope)


def to_near(values, flip):
    ranks = lax.axis_size("sp")
    return lax.ppermute(values, "sp", [(rank, rank ^ flip) for rank in range(ranks)])


def to_high(values, step, ranks):
    if step % (ranks // GROUP) == 0:
        return values
    return lax.ppermute(
        values, "sp", [(rank, (rank + step * GROUP) % ranks) for rank in range(ranks)]
    )


def reorder(blocks, place):
    bit = 1
    while bit < len(blocks):
        swap = place // bit % 2 == 1
        blocks = [jnp.where(swap, blocks[j ^ bit], blocks[j]) for j in range(len(blocks))]
        bit *= 2
    return blocks


def by_distance(values, place):
    return jnp.concatenate(reorder(jnp.split(values, GROUP, axis=1), place), axis=1)


def to_column(values, bit):
    columns = lax.axis_size("tp")
    return lax.ppermute(values, "tp", [(column, column ^ bit) for column in range(columns)])


def gather_columns(values):
    rows = values.shape[0]
    held = {0: values}
    bit = lax.axis_size("tp") // 2
    while bit:
        keys = sorted(held)
        theirs = to_column(jnp.concatenate([held[key] for key in keys], axis=0), bit)
        for at, key in enumerate(keys):
            held[key + bit] = theirs[at * rows : (at + 1) * rows]
        bit //= 2
    return jnp.concatenate([held[key] for key in sorted(held)], axis=0)


def scatter_columns(values):
    columns = lax.axis_size("tp")
    blocks = dict(enumerate(jnp.split(values, columns, axis=0)))
    bit = 1
    while bit < columns:
        mine = [key for key in sorted(blocks) if not key & bit]
        theirs = to_column(jnp.concatenate([blocks[key + bit] for key in mine], axis=0), bit)
        theirs = jnp.split(theirs, len(mine), axis=0)
        blocks = {
            key: (blocks[key].astype(jnp.float32) + piece.astype(jnp.float32)).astype(jnp.bfloat16)
            for key, piece in zip(mine, theirs)
        }
        bit *= 2
    return blocks[0]


def near_weights(gate, up, down):
    gate_one = to_near(gate, 1)
    up_two = to_near(up, 2)
    up_one = to_near(up, 1)
    gate_two = to_near(gate, 2)
    gate_both = to_near(gate_one, 2)
    up_both = to_near(up_two, 1)
    down, gate_both, up_both = lax.optimization_barrier((down, gate_both, up_both))
    half = down.shape[0] // 2
    down_one = to_near(down, 1)
    down_two = to_near(down, 2)
    far = [to_near(down_one[:half], 2), to_near(down_two[half:], 1)]
    down_both = jnp.concatenate(far, axis=0)
    return (
        (gate, gate_one, gate_two, gate_both),
        (up, up_one, up_two, up_both),
        (down, down_one, down_two, down_both),
    )


def blocks_dot(rows, weights, block):
    return sum(
        jnp.dot(
            rows[:, place * block : (place + 1) * block], weight, preferred_element_type=jnp.float32
        )
        for place, weight in enumerate(weights)
    )


def body(
    resid,
    queries,
    latent,
    rope_key,
    lat_gain,
    kv_weight,
    out_gain,
    out_weight,
    ffn_gain,
    gate_weight,
    up_weight,
    down_weight,
):
    gate_blocks, up_blocks, down_blocks = near_weights(gate_weight, up_weight, down_weight)
    rows_here = resid.shape[0]
    first_row = lax.axis_index("sp") * rows_here
    heads_here = queries.shape[1] // (NOPE + ROPE)
    columns = lax.axis_size("tp")
    column = lax.axis_index("tp")
    share = rows_here // columns
    query = jnp.concatenate(reorder(jnp.split(queries, columns, axis=0), column), axis=0)
    query = query.reshape(rows_here, heads_here, NOPE + ROPE)
    within = jnp.arange(rows_here, dtype=jnp.int32)
    own_columns = (within // share) ^ column
    query_index = first_row + own_columns * share + within % share
    query_nope = query[:, :, :NOPE]
    query_rope = rotate(
        query[:, :, NOPE:].astype(jnp.float32), query_index.astype(jnp.float32)[:, None]
    ).astype(jnp.bfloat16)
    scale = 1.0 / math.sqrt(NOPE + ROPE)

    def accumulate(state, key_value, key_rope):
        running_max, running_sum, weighted = state
        length = key_value.shape[0]
        key_value = key_value.reshape(length, heads_here, NOPE + VDIM)
        scores = jnp.einsum(
            "qhd,khd->hqk", query_nope, key_value[:, :, :NOPE], preferred_element_type=jnp.float32
        )
        scores = (
            scores
            + jnp.einsum("qhr,kr->hqk", query_rope, key_rope, preferred_element_type=jnp.float32)
        ) * scale
        allowed = (key_index[None, :] <= query_index[:, None])[None]
        scores = jnp.where(allowed, scores, LOWEST)
        new_max = jnp.maximum(running_max, jnp.max(scores, axis=-1))
        weights = jnp.where(allowed, jnp.exp(scores - new_max[:, :, None]), 0.0)
        running_sum = jnp.sum(weights, axis=-1)
        added = jnp.einsum(
            "hqk,khd->qhd",
            weights.astype(jnp.bfloat16),
            key_value[:, :, NOPE:],
            preferred_element_type=jnp.float32,
        )
        weighted = added
        return (new_max, running_sum, weighted)

    initial = (
        jnp.full((heads_here, rows_here), LOWEST, jnp.float32),
        jnp.zeros((heads_here, rows_here), jnp.float32),
        jnp.zeros((rows_here, heads_here, VDIM), jnp.float32),
    )
    ranks = lax.axis_size("sp")
    rank = lax.axis_index("sp")
    both = jnp.concatenate([latent, rope_key], axis=1)
    both = lax.dynamic_slice_in_dim(both, column * share, share, 0)
    pieces = [both]
    for step in range(1, ranks):
        onward = [(source, source + step) for source in range(ranks - step)]
        pieces.append(lax.ppermute(both, "sp", onward))
    both = gather_columns(jnp.concatenate(pieces, axis=0))
    within = jnp.arange(both.shape[0], dtype=jnp.int32)
    source = (rank - within // share % ranks + ranks) % ranks
    key_index = source * rows_here + ((within // (share * ranks)) ^ column) * share + within % share
    pieces = (both[:, : latent.shape[1]], both[:, latent.shape[1] :])

    def update(state):
        key_value, key_rope = make_keys(pieces[0], pieces[1], lat_gain, kv_weight, key_index)
        return accumulate(state, key_value, key_rope)

    _, running_sum, weighted = update(initial)
    attended = (weighted / jnp.transpose(running_sum)[:, :, None]).astype(jnp.bfloat16)
    attended_float = attended.reshape(rows_here, heads_here * VDIM).astype(jnp.float32)
    squares = jnp.split(jnp.sum(attended_float * attended_float, axis=1), columns)
    squares = lax.psum(jnp.concatenate(reorder(squares, column)), "tp")
    squares = jnp.concatenate(reorder(jnp.split(squares, columns), column))
    normed_out = attended_float * lax.rsqrt(squares / (HEADS * VDIM) + EPSILON)[:, None] * out_gain
    normed_out = normed_out.astype(jnp.bfloat16)
    own_first = lax.axis_index("tp") * share
    projected = jnp.dot(normed_out, out_weight, preferred_element_type=jnp.float32)
    projected = projected.astype(jnp.bfloat16)
    attn_sum = scatter_columns(projected).astype(jnp.float32)
    own_resid = lax.dynamic_slice_in_dim(resid, own_first, share, 0)
    middle = (own_resid.astype(jnp.float32) + attn_sum).astype(jnp.bfloat16)
    highs = ranks // GROUP
    high = rank // GROUP
    place = rank % GROUP
    width = resid.shape[1]
    block = width // ranks
    wide = GROUP * block
    mids = norm_rows(middle, ffn_gain).astype(jnp.bfloat16)
    mids = [
        to_high(
            by_distance(
                lax.dynamic_slice_in_dim(mids, (high + step) % highs * wide, wide, 1), place
            ),
            step,
            ranks,
        )
        for step in range(highs)
    ]
    mids = [gather_columns(piece) for piece in mids]
    gates, ups = None, None
    for step in list(range(1, highs)) + [0]:
        piece = mids[step]
        gate = blocks_dot(piece, gate_blocks, block)
        up = blocks_dot(piece, up_blocks, block)
        if step:
            gate = to_high(gate.astype(jnp.bfloat16), highs - step, ranks).astype(jnp.float32)
            up = to_high(up.astype(jnp.bfloat16), highs - step, ranks).astype(jnp.float32)
        gates = gate if gates is None else gates + gate
        ups = up if ups is None else ups + up
    hidden = (jax.nn.silu(gates) * ups).astype(jnp.bfloat16)
    received = [to_high(hidden, step, ranks) for step in range(highs)]
    terms = []
    for step in range(highs):
        partial = jnp.concatenate(
            [
                jnp.dot(received[step], weight, preferred_element_type=jnp.float32).astype(
                    jnp.bfloat16
                )
                for weight in down_blocks
            ],
            axis=1,
        )
        partial = to_high(scatter_columns(partial), highs - step, ranks)
        terms.append(by_distance(partial, place))
    terms = jnp.concatenate(terms, axis=1)
    ffn_sum = jnp.concatenate(
        [
            lax.dynamic_slice_in_dim(terms, (index - high + highs) % highs * wide, wide, 1)
            for index in range(highs)
        ],
        axis=1,
    ).astype(jnp.float32)
    return (middle.astype(jnp.float32) + ffn_sum).astype(jnp.bfloat16)


def solution(mesh):
    placed = (
        P("sp", None),
        P("sp", "tp"),
        P("sp", None),
        P("sp", None),
        P(),
        P(None, "tp"),
        P("tp"),
        P("tp", None),
        P(),
        P("sp", "tp"),
        P("sp", "tp"),
        P("tp", "sp"),
    )

    return jax.shard_map(
        body, mesh=mesh, in_specs=placed, out_specs=P(("sp", "tp"), None), check_vma=False
    )
```
